32 devices in a mesh: sp: 8 (over z, y), tp: 4 (over x, core).
Axes of the slice: x: 2, y: 2, z: 4, core: 2. Of those that a mesh axis runs over, the one named last changes fastest.
Arguments:
- residual: bfloat16 [3072, 2048], P(('sp', 'tp')), may hold values from -6 to 6
- query_one: bfloat16 [3072, 512], P('sp', 'tp'), may hold values from -6 to 6
- key_one: bfloat16 [3072, 512], P('sp', 'tp'), may hold values from -6 to 6
- value_one: bfloat16 [3072, 1024], P('sp', 'tp'), may hold values from -6 to 6
- gate_one: bfloat16 [3072, 1024], P('sp', 'tp'), may hold values from -6 to 6
- decay_one: bfloat16 [2, 3072, 512], P(None, 'sp', 'tp'), may hold values from -12 to 12
- norm_one: float32 [128], replicated, may hold values from 0.1 to 1.9
- output_one: bfloat16 [1024, 2048], P('tp'), may hold values from -0.125 to 0.125
- query_two: bfloat16 [3072, 1024], P('sp', 'tp'), may hold values from -6 to 6
- key_two: bfloat16 [3072, 1024], P('sp', 'tp'), may hold values from -6 to 6
- value_two: bfloat16 [3072, 1024], P('sp', 'tp'), may hold values from -6 to 6
- gate_two: bfloat16 [3072, 1024], P('sp', 'tp'), may hold values from -6 to 6
- decay_two: bfloat16 [2, 3072, 1024], P(None, 'sp', 'tp'), may hold values from -12 to 12
- norm_two: float32 [128], replicated, may hold values from 0.1 to 1.9
- output_two: bfloat16 [1024, 2048], P('tp'), may hold values from -0.125 to 0.125
- norm_gain: float32 [2048], replicated, may hold values from 0.1 to 1.9
- expert_ids: int32 [3072, 2], P('sp'), may hold values from 0 to 7, as said below
- group_weight: float32 [3072], P('sp'), may hold values from 0.25 to 1
- pair_weight: float32 [3072, 2], P('sp'), may hold values from 0.05 to 1
- expert_gate: bfloat16 [8, 2048, 1024], P('sp', None, 'tp'), may hold values from -0.125 to 0.125
- expert_up: bfloat16 [8, 2048, 1024], P('sp', None, 'tp'), may hold values from -0.125 to 0.125
- expert_down: bfloat16 [8, 1024, 2048], P('sp', 'tp'), may hold values from -0.1875 to 0.1875
Outputs:
- layer_out: bfloat16 [3072, 2048], P(('sp', 'tp'))
The draws below stay inside these ranges and needn't reach their ends.
Inputs may be any that keep to these rules, and one draw needn't show every extreme that they name: `expert_ids`: each row names two different experts of one group, the group of expert e being e // 2. In each aligned block of 96 rows no expert is named more than 49 times, and one expert, the same in every block, is named exactly 49 times in each block.
All inputs are finite; a program needn't handle non-finite values.
Results may differ from the reference program's by a relative error of at most 0.018.
Values may be sent and summed in bfloat16 or wider, within the bound.
A program may use at most 128 MiB of HBM per device.

```python
import math
from functools import partial
import jax
import jax.numpy as jnp
from jax import lax

D = 2048
HEADS_ONE = 8
KEY_ONE = 64
HEADS_TWO = 8
KEY_TWO = 128
VALUE_W = 128
FF = 1024
BLOCK = 64
GROUPS = 4
TOK_DEV = 384
SEQUENCE_TOKENS = 3072
ROWS_DEV = 96
EXPERTS = 8
EXP_GROUP = 2
CAPACITY = 49
N_TP = 4


def decay_law(key, channels):
    random_keys = jax.random.split(key, 6)
    slow = jax.random.uniform(random_keys[0], (2, 1, channels)) < 0.5
    random_jitter = 0.5 * jax.random.normal(random_keys[1], (2, SEQUENCE_TOKENS, channels))
    channel_factor = jnp.exp(jax.random.uniform(random_keys[2], (2, 1, channels), minval=math.log(0.5), maxval=math.log(1.5)))
    device_factor = jnp.exp(jax.random.uniform(random_keys[3], (2, SEQUENCE_TOKENS // TOK_DEV, 1), minval=math.log(0.5), maxval=math.log(1.5)))
    device_factor = jnp.repeat(device_factor, TOK_DEV, axis=1)
    slow_rate = 0.35 * channel_factor * device_factor / SEQUENCE_TOKENS
    fast_rate = 1.0 / (BLOCK * channel_factor)
    rate = jnp.where(slow, slow_rate, fast_rate)
    smoothed_values = -jnp.log(jnp.expm1(16.0 * rate)) + random_jitter
    spike_position = jax.random.randint(random_keys[4], (2, 2, 1), 0, SEQUENCE_TOKENS)
    retained_entries = jax.random.uniform(random_keys[5], (2, 2, 1), minval=0.5, maxval=0.8)
    spike_value = -jnp.log(jnp.expm1(-16.0 * jnp.log(retained_entries)))
    token_positions = jnp.arange(SEQUENCE_TOKENS, dtype=jnp.int32)[None, None, :]
    match_flags = token_positions == spike_position
    spike_row = jnp.sum(jnp.where(match_flags, spike_value, 0.0), axis=1)
    any_match_found = jnp.any(match_flags, axis=1)
    final_output = jnp.where(any_match_found[:, :, None], spike_row[:, :, None] + 0.1 * random_jitter, smoothed_values)
    return jnp.clip(final_output, -12.0, 12.0).astype(jnp.bfloat16)


def draw_decay_one(key, part):
    return decay_law(jax.random.fold_in(key, 11), HEADS_ONE * KEY_ONE)


def draw_decay_two(key, part):
    return decay_law(jax.random.fold_in(key, 12), HEADS_TWO * KEY_TWO)


def route_block(key, hot):
    order_key, group_key, member_key = jax.random.split(key, 3)
    order = jax.random.permutation(order_key, ROWS_DEV).astype(jnp.int32)
    group_score = jax.random.randint(group_key, (ROWS_DEV, GROUPS), 0, 1 << 20) * GROUPS + jnp.arange(GROUPS, dtype=jnp.int32)
    member_score = jax.random.randint(member_key, (ROWS_DEV, EXPERTS), 0, 1 << 20) * EXPERTS + jnp.arange(EXPERTS, dtype=jnp.int32)
    labels = jnp.arange(EXPERTS, dtype=jnp.int32)

    def place_row(counts, step):
        row = order[step]
        forced = step < CAPACITY
        free = counts < CAPACITY
        usable = jnp.sum(free.reshape(GROUPS, EXP_GROUP).astype(jnp.int32), axis=1) >= 2
        picked_group = jnp.argmax(jnp.where(usable, group_score[row], -1)).astype(jnp.int32)
        chosen_group = jnp.where(forced, hot // EXP_GROUP, picked_group)
        allowed = free & (labels // EXP_GROUP == chosen_group)
        scored = jnp.where(allowed, member_score[row], -1)
        first = jnp.where(forced, hot, jnp.argmax(scored).astype(jnp.int32))
        second = jnp.argmax(jnp.where(labels == first, -1, scored)).astype(jnp.int32)
        counts = counts + (labels == first).astype(jnp.int32) + (labels == second).astype(jnp.int32)
        return (counts, (row, first, second))
    _, (rows, firsts, seconds) = lax.scan(place_row, jnp.zeros((EXPERTS,), jnp.int32), jnp.arange(ROWS_DEV, dtype=jnp.int32))
    return jnp.zeros((ROWS_DEV, 2), jnp.int32).at[rows].set(jnp.stack([firsts, seconds], axis=1))


def draw_expert_ids(key, part):
    hot_key, block_key = jax.random.split(jax.random.fold_in(key, 21))
    hot = jax.random.randint(hot_key, (), 0, EXPERTS).astype(jnp.int32)
    random_keys = jax.random.split(block_key, SEQUENCE_TOKENS // ROWS_DEV)
    blocks = jax.vmap(partial(route_block, hot=hot))(random_keys)
    return blocks.reshape(SEQUENCE_TOKENS, 2)


def levels(key, shape, shards, low, high):
    level = 1.0
    for axis_at, shards_of in shards:
        draws = jax.random.uniform(jax.random.fold_in(jax.random.fold_in(key, 6), axis_at), (shards_of,), jnp.float32, low / len(shards), high / len(shards))
        level = level * jnp.repeat(jnp.exp(draws), shape[axis_at] // shards_of).reshape((-1,) + (1,) * (len(shape) - 1 - axis_at))
    return level


def bell_draw(rng, shape, spread, most, shards=(), kind=jnp.bfloat16):
    values = spread * jax.random.normal(rng, shape, jnp.float32)
    if shards:
        values = values * levels(rng, shape, shards, -0.22, 0.18)
    return jnp.clip(values, -most, most).astype(kind)


def setup_inputs(seed: int = 0) -> dict:
    streams_of = jax.random.split(jax.random.key(seed), 23)
    return {
        "residual": bell_draw(streams_of[0], (SEQUENCE_TOKENS, D), 1.0, 6.0, ((0, 32),)),
        "query_one": bell_draw(streams_of[1], (SEQUENCE_TOKENS, HEADS_ONE * KEY_ONE), 1.0, 6.0, ((0, 8), (1, 4))),
        "key_one": bell_draw(streams_of[2], (SEQUENCE_TOKENS, HEADS_ONE * KEY_ONE), 1.0, 6.0, ((0, 8), (1, 4))),
        "value_one": bell_draw(streams_of[3], (SEQUENCE_TOKENS, HEADS_ONE * VALUE_W), 1.0, 6.0, ((0, 8), (1, 4))),
        "gate_one": bell_draw(streams_of[4], (SEQUENCE_TOKENS, HEADS_ONE * VALUE_W), 1.0, 6.0, ((0, 8), (1, 4))),
        "decay_one": draw_decay_one(jax.random.fold_in(streams_of[22], 71), 0),
        "norm_one": jnp.clip(1.0 + 0.18 * jax.random.normal(streams_of[6], (VALUE_W,), jnp.float32), 0.1, 1.9),
        "output_one": bell_draw(streams_of[7], (HEADS_ONE * VALUE_W, D), ((HEADS_ONE + HEADS_TWO) * VALUE_W) ** -0.5, 0.125, ((0, 4),)),
        "query_two": bell_draw(streams_of[8], (SEQUENCE_TOKENS, HEADS_TWO * KEY_TWO), 1.0, 6.0, ((0, 8), (1, 4))),
        "key_two": bell_draw(streams_of[9], (SEQUENCE_TOKENS, HEADS_TWO * KEY_TWO), 1.0, 6.0, ((0, 8), (1, 4))),
        "value_two": bell_draw(streams_of[10], (SEQUENCE_TOKENS, HEADS_TWO * VALUE_W), 1.0, 6.0, ((0, 8), (1, 4))),
        "gate_two": bell_draw(streams_of[11], (SEQUENCE_TOKENS, HEADS_TWO * VALUE_W), 1.0, 6.0, ((0, 8), (1, 4))),
        "decay_two": draw_decay_two(jax.random.fold_in(streams_of[22], 71), 0),
        "norm_two": jnp.clip(1.0 + 0.18 * jax.random.normal(streams_of[13], (VALUE_W,), jnp.float32), 0.1, 1.9),
        "output_two": bell_draw(streams_of[14], (HEADS_TWO * VALUE_W, D), ((HEADS_ONE + HEADS_TWO) * VALUE_W) ** -0.5, 0.125, ((0, 4),)),
        "norm_gain": jnp.clip(1.0 + 0.18 * jax.random.normal(streams_of[15], (D,), jnp.float32), 0.1, 1.9),
        "expert_ids": draw_expert_ids(jax.random.fold_in(streams_of[22], 71), 0),
        "group_weight": jnp.clip(jnp.exp(math.log(1.0) - 1.3862944 * jax.random.uniform(streams_of[17], (SEQUENCE_TOKENS,), jnp.float32) ** levels(streams_of[17], (SEQUENCE_TOKENS,), ((0, 8),), -0.2, 0.2)), 0.25, 1.0),
        "pair_weight": jnp.clip(jnp.exp(math.log(1.0) - 2.9957323 * jax.random.uniform(streams_of[18], (SEQUENCE_TOKENS, 2), jnp.float32) ** levels(streams_of[18], (SEQUENCE_TOKENS, 2), ((0, 8),), -0.2, 0.2)), 0.05, 1.0),
        "expert_gate": bell_draw(streams_of[19], (EXPERTS, D, FF), D ** -0.5, 0.125, ((0, 8), (2, 4))),
        "expert_up": bell_draw(streams_of[20], (EXPERTS, D, FF), D ** -0.5, 0.125, ((0, 8), (2, 4))),
        "expert_down": bell_draw(streams_of[21], (EXPERTS, FF, D), FF ** -0.5, 0.1875, ((0, 8), (1, 4))),
    }


HIGH = lax.Precision.HIGHEST
TAU = 16.0
EPS = 1e-06

def advance(state_now, step_input):
    fade_rate, extra_term = step_input
    return (fade_rate[..., None] * state_now + extra_term, state_now)

def block_pass(queries, key_rows, values, rates):
    length, heads, width = queries.shape
    blocks = length // BLOCK
    shaped = (blocks, BLOCK, heads, width)
    cumul = jnp.cumsum(rates.reshape(shaped), axis=1)
    block_end = cumul[:, -1]
    key_blocks = key_rows.reshape(shaped)
    value_blocks = values.reshape(blocks, BLOCK, heads, values.shape[-1])
    query_dec = queries.reshape(shaped) * jnp.exp(cumul)
    query_low = query_dec.astype(jnp.bfloat16)
    key_dec = (key_blocks * jnp.exp(-cumul)).astype(jnp.bfloat16)
    key_end = (key_blocks * jnp.exp(block_end[:, None] - cumul)).astype(jnp.bfloat16)
    lower_mask = jnp.tril(jnp.ones((BLOCK, BLOCK), jnp.float32))
    scores = jnp.einsum('nthd,nshd->nhts', query_low, key_dec, preferred_element_type=jnp.float32) * lower_mask
    scores = scores.astype(jnp.bfloat16)
    inner_part = jnp.einsum('nhts,nshe->nthe', scores, value_blocks, preferred_element_type=jnp.float32)
    added = jnp.einsum('nshd,nshe->nhde', key_end, value_blocks, preferred_element_type=jnp.float32)
    empty = jnp.zeros((heads, width, values.shape[-1]), jnp.float32)
    state_out, before = lax.scan(advance, empty, (jnp.exp(block_end), added))
    outer_part = jnp.einsum('nthd,nhde->nthe', query_dec, before, precision=HIGH)
    return (inner_part + outer_part).reshape(length, heads, values.shape[-1])

def group_mix(query, key_in, value, gate, decay, gain, width):
    heads = query.shape[1] // width
    queries = query.astype(jnp.float32).reshape(SEQUENCE_TOKENS, heads, width) * width ** (-0.5)
    key_rows = key_in.astype(jnp.float32).reshape(SEQUENCE_TOKENS, heads, width)
    values = value.reshape(SEQUENCE_TOKENS, heads, VALUE_W)
    rates = jax.nn.log_sigmoid(decay.astype(jnp.float32)) / TAU
    ahead = block_pass(queries, key_rows, values, rates[0].reshape(SEQUENCE_TOKENS, heads, width))
    behind = block_pass(jnp.flip(queries, 0), jnp.flip(key_rows, 0), jnp.flip(values, 0), jnp.flip(rates[1], 0).reshape(SEQUENCE_TOKENS, heads, width))
    total = ahead + jnp.flip(behind, 0)
    scale = lax.rsqrt(lax.optimization_barrier(jnp.mean(total * total, axis=-1, keepdims=True)) + EPS)
    normed = (total * scale * gain).reshape(SEQUENCE_TOKENS, heads * VALUE_W)
    return (normed * jax.nn.silu(gate.astype(jnp.float32))).astype(jnp.bfloat16)

def rounded(term):
    return lax.optimization_barrier(term.astype(jnp.bfloat16)).astype(jnp.float32)

def slot_table(routes, capacity, experts):
    flat = routes.reshape(-1)
    count = flat.shape[0]
    onehot = (flat[:, None] == jnp.arange(experts, dtype=jnp.int32)[None, :]).astype(jnp.int32)
    place = lax.optimization_barrier(jnp.sum((jnp.cumsum(onehot, axis=0) - onehot) * onehot, axis=1)).astype(jnp.int32)
    table = jnp.full((experts, capacity), count, jnp.int32).at[flat, place].set(jnp.arange(count, dtype=jnp.int32))
    return (table, place)

def reference(residual, query_one, key_one, value_one, gate_one, decay_one, norm_one, output_one, query_two, key_two, value_two, gate_two, decay_two, norm_two, output_two, norm_gain, expert_ids, group_weight, pair_weight, expert_gate, expert_up, expert_down):
    mixed_one = group_mix(query_one, key_one, value_one, gate_one, decay_one, norm_one, KEY_ONE)
    mixed_two = group_mix(query_two, key_two, value_two, gate_two, decay_two, norm_two, KEY_TWO)
    span_one = mixed_one.shape[1] // N_TP
    span_two = mixed_two.shape[1] // N_TP
    projected = jnp.zeros((SEQUENCE_TOKENS, D), jnp.float32)
    for part in range(N_TP):
        term = jnp.dot(mixed_one[:, part * span_one:(part + 1) * span_one], output_one[part * span_one:(part + 1) * span_one], preferred_element_type=jnp.float32)
        term = term + jnp.dot(mixed_two[:, part * span_two:(part + 1) * span_two], output_two[part * span_two:(part + 1) * span_two], preferred_element_type=jnp.float32)
        projected = projected + rounded(term)
    stream = (residual.astype(jnp.float32) + rounded(projected)).astype(jnp.bfloat16)
    wide = stream.astype(jnp.float32)
    normed = (wide * lax.rsqrt(lax.optimization_barrier(jnp.mean(wide * wide, axis=-1, keepdims=True)) + EPS) * norm_gain).astype(jnp.bfloat16)
    weights = group_weight[:, None] * pair_weight / lax.optimization_barrier(jnp.sum(pair_weight, axis=1, keepdims=True))
    blocks = SEQUENCE_TOKENS // ROWS_DEV
    tables, places = jax.vmap(partial(slot_table, capacity=CAPACITY, experts=EXPERTS))(expert_ids.reshape(blocks, ROWS_DEV, 2))
    offsets = (jnp.arange(blocks, dtype=jnp.int32) * (2 * ROWS_DEV))[:, None, None]
    assigned = jnp.where(tables == 2 * ROWS_DEV, 2 * SEQUENCE_TOKENS, tables + offsets).astype(jnp.int32)
    assigned = jnp.transpose(assigned, (1, 0, 2)).reshape(EXPERTS, blocks * CAPACITY)
    padded = jnp.concatenate([normed, jnp.zeros((1, D), jnp.bfloat16)], axis=0)
    route_weight = jnp.concatenate([weights.reshape(-1), jnp.zeros((1,), jnp.float32)])
    span = FF // N_TP

    def expert_pass(total, step_input):
        index, weight_gate, weight_up, weight_down = step_input
        token = index // 2
        rows = padded[token]
        gate_part = jnp.dot(rows, weight_gate, preferred_element_type=jnp.float32)
        up_part = jnp.dot(rows, weight_up, preferred_element_type=jnp.float32)
        hidden = (jax.nn.silu(gate_part) * up_part).astype(jnp.bfloat16)
        summed = jnp.zeros((rows.shape[0], D), jnp.float32)
        for part in range(N_TP):
            summed = summed + rounded(jnp.dot(hidden[:, part * span:(part + 1) * span], weight_down[part * span:(part + 1) * span], preferred_element_type=jnp.float32))
        final_output = rounded(summed)
        return (total.at[token].add(route_weight[index][:, None] * final_output), None)
    total, _ = lax.scan(expert_pass, jnp.zeros((SEQUENCE_TOKENS + 1, D), jnp.float32), (assigned, expert_gate, expert_up, expert_down))
    return (stream.astype(jnp.float32) + total[:SEQUENCE_TOKENS]).astype(jnp.bfloat16)
```

```python
import functools

import jax
import jax.numpy as jnp
from jax import lax
from jax.experimental import pallas as pl
from jax.experimental.pallas import tpu as pltpu
from jax.sharding import PartitionSpec as P

D = 2048
KEY_ONE = 64
KEY_TWO = 128
VALUE_W = 128
BLOCK = 64
GROUPS = 4


MESH = pl.DeviceIdType.MESH
TAU = 16.0
EPS = 1e-06


def log_sigmoid(x):
    return jnp.minimum(x, 0.0) - jnp.log1p(jnp.exp(-jnp.abs(x)))


def contract(a, b, dims):
    return lax.dot_general(a, b, (dims, ((), ())), preferred_element_type=jnp.float32)


NN, NT, TN = ((1,), (0,)), ((1,), (1,)), ((0,), (0,))


def flip_bit(index, bit):
    return index + bit - 2 * bit * lax.rem(index // bit, 2)


def meet(peers):
    barrier = pltpu.get_barrier_semaphore()
    for peer in peers:
        pl.semaphore_signal(barrier, inc=1, device_id=peer, device_id_type=MESH)
    pl.semaphore_wait(barrier, len(peers))


def mixer_kernel(
    n_sp,
    n_tp,
    q1,
    k1,
    v1,
    g1,
    d1,
    q2,
    k2,
    v2,
    g2,
    d2,
    norm1,
    norm2,
    out1,
    out2,
    res,
    gain,
    stream_ref,
    normed_ref,
    cum,
    qd,
    kd,
    added,
    ends,
    sent,
    got,
    carried,
    total,
    mixed,
    part_send,
    part_got,
    st_send,
    st_recv,
    pt_send,
    pt_recv,
):
    sp, tp = lax.axis_index("sp"), lax.axis_index("tp")
    length = q1.shape[0]
    blocks = length // BLOCK
    lanes = 128
    units = []
    for q, k, v, g, d, norm, key in (
        (q1, k1, v1, g1, d1, norm1, KEY_ONE),
        (q2, k2, v2, g2, d2, norm2, KEY_TWO),
    ):
        per = lanes // key
        for at in range(q.shape[1] // lanes):
            units.append((q, k, v, g, d, norm, key, per, at))
    count = len(units)
    bits = [1 << r for r in range(n_tp.bit_length() - 1)]

    meet(
        [(lax.rem(sp + off, n_sp), tp) for off in range(1, n_sp)]
        + [(sp, flip_bit(tp, bit)) for bit in bits]
    )

    t_at = lax.broadcasted_iota(jnp.int32, (length, length), 0)
    s_at = lax.broadcasted_iota(jnp.int32, (length, length), 1)
    same = (t_at // BLOCK) == (s_at // BLOCK)
    for way in range(2):
        tri = jnp.where(same & ((s_at <= t_at) if way == 0 else (s_at >= t_at)), 1.0, 0.0).astype(
            jnp.bfloat16
        )
        for u, (q, k, v, g, d, norm, key, per, at) in enumerate(units):
            cols = slice(at * lanes, (at + 1) * lanes)
            rate = log_sigmoid(d[way, :, cols].astype(jnp.float32)) / TAU
            high = rate.astype(jnp.bfloat16)
            rest = rate - high.astype(jnp.float32)
            mid = rest.astype(jnp.bfloat16)
            low = (rest - mid.astype(jnp.float32)).astype(jnp.bfloat16)
            cum[u] = contract(tri, high, NN) + contract(tri, mid, NN) + contract(tri, low, NN)
            state = jnp.zeros((VALUE_W, lanes), jnp.float32)
            reach = jnp.zeros((1, lanes), jnp.float32)
            lane = lax.broadcasted_iota(jnp.int32, (VALUE_W, lanes), 1) // key
            for n in range(blocks) if way == 0 else range(blocks - 1, -1, -1):
                rows = slice(n * BLOCK, (n + 1) * BLOCK)
                c = cum[u, rows, :]
                e = c[BLOCK - 1 : BLOCK] if way == 0 else c[0:1]
                queries = q[rows, cols].astype(jnp.float32) * key ** (-0.5)
                keys = k[rows, cols].astype(jnp.float32)
                qd[way, u, rows, :] = (queries * jnp.exp(c)).astype(jnp.bfloat16)
                kd[way, u, rows, :] = (keys * jnp.exp(-c)).astype(jnp.bfloat16)
                end = (keys * jnp.exp(e - c)).astype(jnp.bfloat16)
                term = None
                for h in range(per):
                    head = at * per + h
                    value = v[rows, head * VALUE_W : (head + 1) * VALUE_W]
                    new = contract(value, end, TN)
                    term = new if term is None else jnp.where(lane == h, new, term)
                added[way, u, n] = term
                fade = jnp.exp(e)
                ends[way, u, n : n + 1, :] = fade
                state = state * fade + term
                reach = reach + e
            sent[way, u * VALUE_W : (u + 1) * VALUE_W, :] = state.astype(jnp.bfloat16)
            sent[way, count * VALUE_W + 16 * u : count * VALUE_W + 16 * (u + 1), :] = (
                jnp.broadcast_to(jnp.exp(reach), (16, lanes)).astype(jnp.bfloat16)
            )

    def state_copy(off):
        to = lax.rem(sp + off, n_sp)
        way = jnp.where(to > sp, 0, 1)
        return pltpu.make_async_remote_copy(
            src_ref=sent.at[way],
            dst_ref=got.at[off],
            send_sem=st_send.at[off],
            recv_sem=st_recv.at[off],
            device_id=(to, tp),
            device_id_type=MESH,
        )

    @pl.loop(1, n_sp)
    def _(off):
        state_copy(off).start()

    t_blk = lax.broadcasted_iota(jnp.int32, (BLOCK, BLOCK), 0)
    s_blk = lax.broadcasted_iota(jnp.int32, (BLOCK, BLOCK), 1)
    first = 0
    for u, (q, k, v, g, d, norm, key, per, at) in enumerate(units):
        lane = lax.broadcasted_iota(jnp.int32, (BLOCK, lanes), 1) // key
        for h in range(per):
            head = at * per + h
            for n in range(blocks):
                rows = slice(n * BLOCK, (n + 1) * BLOCK)
                scores = None
                for way in range(2):
                    queries = qd[way, u, rows, :]
                    if per > 1:
                        queries = jnp.where(lane == h, queries, jnp.zeros_like(queries))
                    one = contract(queries, kd[way, u, rows, :], NT)
                    one = jnp.where((s_blk <= t_blk) if way == 0 else (s_blk >= t_blk), one, 0.0)
                    scores = one if scores is None else scores + one
                value = v[rows, head * VALUE_W : (head + 1) * VALUE_W]
                total[first + h, rows, :] = contract(scores.astype(jnp.bfloat16), value, NN)
        first += per

    @pl.loop(1, n_sp)
    def _(off):
        state_copy(off).wait()

    carried[...] = jnp.zeros_like(carried)

    def fold(way, who):
        off = lax.rem(sp - who + n_sp, n_sp)
        for u in range(count):
            fade = got[off, count * VALUE_W + 16 * u : count * VALUE_W + 16 * (u + 1), :][0:1]
            state = got[off, u * VALUE_W : (u + 1) * VALUE_W, :]
            carried[way, u] = carried[way, u] * fade.astype(jnp.float32) + state.astype(jnp.float32)

    @pl.loop(0, sp)
    def _(who):
        fold(0, who)

    @pl.loop(0, n_sp - 1 - sp)
    def _(back):
        fold(1, n_sp - 1 - back)

    first = 0
    for u, (q, k, v, g, d, norm, key, per, at) in enumerate(units):
        lane = lax.broadcasted_iota(jnp.int32, (BLOCK, lanes), 1) // key
        for way in range(2):
            state = carried[way, u]
            for n in range(blocks) if way == 0 else range(blocks - 1, -1, -1):
                rows = slice(n * BLOCK, (n + 1) * BLOCK)
                low = state.astype(jnp.bfloat16)
                for h in range(per):
                    queries = qd[way, u, rows, :]
                    if per > 1:
                        queries = jnp.where(lane == h, queries, jnp.zeros_like(queries))
                    total[first + h, rows, :] += contract(queries, low, NT)
                state = state * ends[way, u, n : n + 1, :] + added[way, u, n]
        for h in range(per):
            head = at * per + h
            cols = slice(head * VALUE_W, (head + 1) * VALUE_W)
            x = total[first + h]
            y = x * lax.rsqrt(jnp.mean(x * x, axis=-1, keepdims=True) + EPS) * norm[...]
            gate = g[:, cols].astype(jnp.float32)
            y = y * (gate / (1.0 + jnp.exp(-gate)))
            mixed[:, (first + h) * VALUE_W : (first + h + 1) * VALUE_W] = y.astype(jnp.bfloat16)
        first += per

    rows_dev = res.shape[0]
    split = out1.shape[0]

    def project(mask):
        block = tp
        for bit in bits:
            if mask & bit:
                block = flip_bit(block, bit)
        rows = pl.ds(pl.multiple_of(block * rows_dev, 16), rows_dev)
        return contract(mixed[rows, :split], out1[...], NN) + contract(
            mixed[rows, split:], out2[...], NN
        )

    def part_copy(mask, bit):
        return pltpu.make_async_remote_copy(
            src_ref=part_send.at[mask],
            dst_ref=part_got.at[mask],
            send_sem=pt_send.at[mask],
            recv_sem=pt_recv.at[mask],
            device_id=(sp, flip_bit(tp, bit)),
            device_id_type=MESH,
        )

    low_bit = lambda m: m & -m
    order = sorted(range(1, n_tp), key=lambda m: (low_bit(m), -m))
    for mask in order:
        bit = low_bit(mask)
        value = project(mask)
        for earlier in bits:
            if earlier < bit:
                part_copy(mask | earlier, earlier).wait_recv()
                value = value + part_got[mask | earlier].astype(jnp.float32)
        part_send[mask] = value.astype(jnp.bfloat16)
        part_copy(mask, bit).start()
    value = project(0)
    for bit in bits:
        part_copy(bit, bit).wait_recv()
        value = value + part_got[bit].astype(jnp.float32)
    stream = (res[...].astype(jnp.float32) + value.astype(jnp.bfloat16).astype(jnp.float32)).astype(
        jnp.bfloat16
    )
    stream_ref[...] = stream
    wide = stream.astype(jnp.float32)
    scale = lax.rsqrt(jnp.mean(wide * wide, axis=-1, keepdims=True) + EPS)
    normed_ref[...] = (wide * scale * gain[...]).astype(jnp.bfloat16)
    for mask in order:
        part_copy(mask, low_bit(mask)).wait_send()


def mixer(n_sp, n_tp, args, residual, norm_gain):
    q1, k1, v1, g1, d1, norm1, out1, q2, k2, v2, g2, d2, norm2, out2 = args
    length = q1.shape[0]
    blocks = length // BLOCK
    count = (q1.shape[1] + q2.shape[1]) // 128
    heads = (v1.shape[1] + v2.shape[1]) // VALUE_W
    rows, width = residual.shape
    packed = count * (VALUE_W + 16)
    bf, f32 = jnp.bfloat16, jnp.float32
    vmem = pl.BlockSpec(memory_space=pltpu.VMEM)
    sem = pltpu.SemaphoreType.DMA
    return pl.pallas_call(
        functools.partial(mixer_kernel, n_sp, n_tp),
        out_shape=(jax.ShapeDtypeStruct((rows, width), bf),) * 2,
        in_specs=[vmem] * 16,
        out_specs=(vmem, vmem),
        scratch_shapes=[
            pltpu.VMEM((count, length, 128), f32),
            pltpu.VMEM((2, count, length, 128), bf),
            pltpu.VMEM((2, count, length, 128), bf),
            pltpu.VMEM((2, count, blocks, VALUE_W, 128), f32),
            pltpu.VMEM((2, count, -(-blocks // 8) * 8, 128), f32),
            pltpu.VMEM((2, packed, 128), bf),
            pltpu.VMEM((n_sp, packed, 128), bf),
            pltpu.VMEM((2, count, VALUE_W, 128), f32),
            pltpu.VMEM((heads, length, VALUE_W), f32),
            pltpu.VMEM((length, heads * VALUE_W), bf),
            pltpu.VMEM((n_tp, rows, width), bf),
            pltpu.VMEM((n_tp, rows, width), bf),
            sem((n_sp,)),
            sem((n_sp,)),
            sem((n_tp,)),
            sem((n_tp,)),
        ],
        compiler_params=pltpu.CompilerParams(
            collective_id=0, has_side_effects=True, vmem_limit_bytes=60 * 2**20
        ),
    )(
        q1, k1, v1, g1, d1, q2, k2, v2, g2, d2,
        norm1[None], norm2[None], out1, out2, residual, norm_gain[None],
    )


def slot_table(routes, capacity, experts):
    flat = routes.reshape(-1)
    count = flat.shape[0]
    onehot = (flat[:, None] == jnp.arange(experts, dtype=jnp.int32)[None, :]).astype(jnp.int32)
    place = jnp.sum((jnp.cumsum(onehot, axis=0) - onehot) * onehot, axis=1)
    table = (
        jnp.full((experts, capacity), count, jnp.int32)
        .at[flat, place]
        .set(jnp.arange(count, dtype=jnp.int32))
    )
    return (table, place)


def body(
    residual,
    query_one,
    key_one,
    value_one,
    gate_one,
    decay_one,
    norm_one,
    output_one,
    query_two,
    key_two,
    value_two,
    gate_two,
    decay_two,
    norm_two,
    output_two,
    norm_gain,
    expert_ids,
    group_weight,
    pair_weight,
    expert_gate,
    expert_up,
    expert_down,
):
    stream, normed_rows = mixer(
        lax.axis_size("sp"),
        lax.axis_size("tp"),
        (
            query_one, key_one, value_one, gate_one, decay_one, norm_one, output_one,
            query_two, key_two, value_two, gate_two, decay_two, norm_two, output_two,
        ),
        residual,
        norm_gain,
    )
    rows_dev = residual.shape[0]
    rank = lax.axis_index("tp")
    experts = lax.axis_size("sp")
    capacity = max(2, 2 * rows_dev // (experts - GROUPS) + 1)
    own_routes = lax.dynamic_slice_in_dim(expert_ids, rank * rows_dev, rows_dev, 0)
    own_group = lax.dynamic_slice_in_dim(group_weight, rank * rows_dev, rows_dev, 0)
    own_pair = lax.dynamic_slice_in_dim(pair_weight, rank * rows_dev, rows_dev, 0)
    weights = own_group[:, None] * own_pair / jnp.sum(own_pair, axis=1, keepdims=True)
    blank = jnp.zeros((1, D), jnp.bfloat16)
    table, own_place = slot_table(own_routes, capacity, experts)
    index = jnp.where(table == 2 * rows_dev, rows_dev, table // 2)
    send = jnp.concatenate([normed_rows, blank], axis=0)[index][None]
    received = lax.all_to_all(send, "sp", split_axis=1, concat_axis=1, tiled=True)
    received = lax.all_gather(received, "tp", axis=0, tiled=True)
    flat = received.reshape(-1, received.shape[-1])
    gate_part = jnp.dot(flat, expert_gate[0], preferred_element_type=jnp.float32)
    up_part = jnp.dot(flat, expert_up[0], preferred_element_type=jnp.float32)
    hidden = (jax.nn.silu(gate_part) * up_part).astype(jnp.bfloat16)
    share_sum = lax.psum_scatter(
        jnp.dot(hidden, expert_down[0], preferred_element_type=jnp.float32)
        .reshape(received.shape)
        .astype(jnp.bfloat16),
        "tp",
        scatter_dimension=0,
        tiled=True,
    )
    returned = lax.all_to_all(share_sum, "sp", split_axis=1, concat_axis=1, tiled=True)
    slot_index = own_routes.reshape(-1) * capacity + own_place
    picked = returned.reshape(-1, D)[slot_index].astype(jnp.float32).reshape(rows_dev, 2, D)
    layer = stream.astype(jnp.float32) + jnp.sum(weights[:, :, None] * picked, axis=1)
    return layer.astype(jnp.bfloat16)


def solution(mesh):
    placed = (
        P(("sp", "tp"), None),
        P("sp", "tp"),
        P("sp", "tp"),
        P("sp", "tp"),
        P("sp", "tp"),
        P(None, "sp", "tp"),
        P(),
        P("tp", None),
        P("sp", "tp"),
        P("sp", "tp"),
        P("sp", "tp"),
        P("sp", "tp"),
        P(None, "sp", "tp"),
        P(),
        P("tp", None),
        P(),
        P("sp", None),
        P("sp"),
        P("sp", None),
        P("sp", None, "tp"),
        P("sp", None, "tp"),
        P("sp", "tp", None),
    )
    return jax.shard_map(
        body, mesh=mesh, in_specs=placed, out_specs=P(("sp", "tp"), None), check_vma=False
    )
```

```python
import functools

import jax
import jax.numpy as jnp
from jax import lax
from jax.experimental import pallas as pl
from jax.experimental.pallas import tpu as pltpu
from jax.sharding import PartitionSpec as P

D = 2048
KEY_ONE = 64
KEY_TWO = 128
VALUE_W = 128
BLOCK = 64
GROUPS = 4


MESH = pl.DeviceIdType.MESH
TAU = 16.0
EPS = 1e-06


def log_sigmoid(x):
    return jnp.minimum(x, 0.0) - jnp.log1p(jnp.exp(-jnp.abs(x)))


def contract(a, b, dims):
    return lax.dot_general(a, b, (dims, ((), ())), preferred_element_type=jnp.float32)


NN, NT, TN = ((1,), (0,)), ((1,), (1,)), ((0,), (0,))


def flip_bit(index, bit):
    return index + bit - 2 * bit * lax.rem(index // bit, 2)


def meet(peers):
    barrier = pltpu.get_barrier_semaphore()
    for peer in peers:
        pl.semaphore_signal(barrier, inc=1, device_id=peer, device_id_type=MESH)
    pl.semaphore_wait(barrier, len(peers))


def mixer_kernel(
    n_sp,
    n_tp,
    q1,
    k1,
    v1,
    g1,
    d1,
    q2,
    k2,
    v2,
    g2,
    d2,
    norm1,
    norm2,
    out1,
    out2,
    res,
    gain,
    stream_ref,
    normed_ref,
    cum,
    qd,
    kd,
    added,
    ends,
    sent,
    got,
    carried,
    total,
    mixed,
    part_send,
    part_got,
    st_send,
    st_recv,
    pt_send,
    pt_recv,
):
    sp, tp = lax.axis_index("sp"), lax.axis_index("tp")
    length = q1.shape[0]
    blocks = length // BLOCK
    lanes = 128
    units = []
    for q, k, v, g, d, norm, key in (
        (q1, k1, v1, g1, d1, norm1, KEY_ONE),
        (q2, k2, v2, g2, d2, norm2, KEY_TWO),
    ):
        per = lanes // key
        for at in range(q.shape[1] // lanes):
            units.append((q, k, v, g, d, norm, key, per, at))
    count = len(units)
    bits = [1 << r for r in range(n_tp.bit_length() - 1)]

    meet(
        [(lax.rem(sp + off, n_sp), tp) for off in range(1, n_sp)]
        + [(sp, flip_bit(tp, bit)) for bit in bits]
    )

    t_at = lax.broadcasted_iota(jnp.int32, (length, length), 0)
    s_at = lax.broadcasted_iota(jnp.int32, (length, length), 1)
    same = (t_at // BLOCK) == (s_at // BLOCK)
    for way in range(2):
        tri = jnp.where(same & ((s_at <= t_at) if way == 0 else (s_at >= t_at)), 1.0, 0.0).astype(
            jnp.bfloat16
        )
        for u, (q, k, v, g, d, norm, key, per, at) in enumerate(units):
            cols = slice(at * lanes, (at + 1) * lanes)
            rate = log_sigmoid(d[way, :, cols].astype(jnp.float32)) / TAU
            high = rate.astype(jnp.bfloat16)
            rest = rate - high.astype(jnp.float32)
            mid = rest.astype(jnp.bfloat16)
            low = (rest - mid.astype(jnp.float32)).astype(jnp.bfloat16)
            cum[u] = contract(tri, high, NN) + contract(tri, mid, NN) + contract(tri, low, NN)
            state = jnp.zeros((VALUE_W, lanes), jnp.float32)
            reach = jnp.zeros((1, lanes), jnp.float32)
            lane = lax.broadcasted_iota(jnp.int32, (VALUE_W, lanes), 1) // key
            for n in range(blocks) if way == 0 else range(blocks - 1, -1, -1):
                rows = slice(n * BLOCK, (n + 1) * BLOCK)
                c = cum[u, rows, :]
                e = c[BLOCK - 1 : BLOCK] if way == 0 else c[0:1]
                queries = q[rows, cols].astype(jnp.float32) * key ** (-0.5)
                keys = k[rows, cols].astype(jnp.float32)
                qd[way, u, rows, :] = (queries * jnp.exp(c)).astype(jnp.bfloat16)
                kd[way, u, rows, :] = (keys * jnp.exp(-c)).astype(jnp.bfloat16)
                end = (keys * jnp.exp(e - c)).astype(jnp.bfloat16)
                term = None
                for h in range(per):
                    head = at * per + h
                    value = v[rows, head * VALUE_W : (head + 1) * VALUE_W]
                    new = contract(value, end, TN)
                    term = new if term is None else jnp.where(lane == h, new, term)
                added[way, u, n] = term
                fade = jnp.exp(e)
                ends[way, u, n : n + 1, :] = fade
                state = state * fade + term
                reach = reach + e
            sent[way, u * VALUE_W : (u + 1) * VALUE_W, :] = state.astype(jnp.bfloat16)
            sent[way, count * VALUE_W + 16 * u : count * VALUE_W + 16 * (u + 1), :] = (
                jnp.broadcast_to(jnp.exp(reach), (16, lanes)).astype(jnp.bfloat16)
            )

    def state_copy(off):
        to = lax.rem(sp + off, n_sp)
        way = jnp.where(to > sp, 0, 1)
        return pltpu.make_async_remote_copy(
            src_ref=sent.at[way],
            dst_ref=got.at[off],
            send_sem=st_send.at[off],
            recv_sem=st_recv.at[off],
            device_id=(to, tp),
            device_id_type=MESH,
        )

    @pl.loop(1, n_sp)
    def _(off):
        state_copy(off).start()

    t_blk = lax.broadcasted_iota(jnp.int32, (BLOCK, BLOCK), 0)
    s_blk = lax.broadcasted_iota(jnp.int32, (BLOCK, BLOCK), 1)
    first = 0
    for u, (q, k, v, g, d, norm, key, per, at) in enumerate(units):
        lane = lax.broadcasted_iota(jnp.int32, (BLOCK, lanes), 1) // key
        for h in range(per):
            head = at * per + h
            for n in range(blocks):
                rows = slice(n * BLOCK, (n + 1) * BLOCK)
                scores = None
                for way in range(2):
                    queries = qd[way, u, rows, :]
                    if per > 1:
                        queries = jnp.where(lane == h, queries, jnp.zeros_like(queries))
                    one = contract(queries, kd[way, u, rows, :], NT)
                    one = jnp.where((s_blk <= t_blk) if way == 0 else (s_blk >= t_blk), one, 0.0)
                    scores = one if scores is None else scores + one
                value = v[rows, head * VALUE_W : (head + 1) * VALUE_W]
                total[first + h, rows, :] = contract(scores.astype(jnp.bfloat16), value, NN)
        first += per

    @pl.loop(1, n_sp)
    def _(off):
        state_copy(off).wait()

    carried[...] = jnp.zeros_like(carried)

    def fold(way, who):
        off = lax.rem(sp - who + n_sp, n_sp)
        for u in range(count):
            fade = got[off, count * VALUE_W + 16 * u : count * VALUE_W + 16 * (u + 1), :][0:1]
            state = got[off, u * VALUE_W : (u + 1) * VALUE_W, :]
            carried[way, u] = carried[way, u] * fade.astype(jnp.float32) + state.astype(jnp.float32)

    @pl.loop(0, sp)
    def _(who):
        fold(0, who)

    @pl.loop(0, n_sp - 1 - sp)
    def _(back):
        fold(1, n_sp - 1 - back)

    first = 0
    for u, (q, k, v, g, d, norm, key, per, at) in enumerate(units):
        lane = lax.broadcasted_iota(jnp.int32, (BLOCK, lanes), 1) // key
        for way in range(2):
            state = carried[way, u]
            for n in range(blocks) if way == 0 else range(blocks - 1, -1, -1):
                rows = slice(n * BLOCK, (n + 1) * BLOCK)
                low = state.astype(jnp.bfloat16)
                for h in range(per):
                    queries = qd[way, u, rows, :]
                    if per > 1:
                        queries = jnp.where(lane == h, queries, jnp.zeros_like(queries))
                    total[first + h, rows, :] += contract(queries, low, NT)
                state = state * ends[way, u, n : n + 1, :] + added[way, u, n]
        for h in range(per):
            head = at * per + h
            cols = slice(head * VALUE_W, (head + 1) * VALUE_W)
            x = total[first + h]
            y = x * lax.rsqrt(jnp.mean(x * x, axis=-1, keepdims=True) + EPS) * norm[...]
            gate = g[:, cols].astype(jnp.float32)
            y = y * (gate / (1.0 + jnp.exp(-gate)))
            mixed[:, (first + h) * VALUE_W : (first + h + 1) * VALUE_W] = y.astype(jnp.bfloat16)
        first += per

    rows_dev = res.shape[0]
    split = out1.shape[0]

    def project(mask):
        block = tp
        for bit in bits:
            if mask & bit:
                block = flip_bit(block, bit)
        rows = pl.ds(pl.multiple_of(block * rows_dev, 16), rows_dev)
        return contract(mixed[rows, :split], out1[...], NN) + contract(
            mixed[rows, split:], out2[...], NN
        )

    def part_copy(mask, bit):
        return pltpu.make_async_remote_copy(
            src_ref=part_send.at[mask],
            dst_ref=part_got.at[mask],
            send_sem=pt_send.at[mask],
            recv_sem=pt_recv.at[mask],
            device_id=(sp, flip_bit(tp, bit)),
            device_id_type=MESH,
        )

    low_bit = lambda m: m & -m
    order = sorted(range(1, n_tp), key=lambda m: (low_bit(m), -m))
    for mask in order:
        bit = low_bit(mask)
        value = project(mask)
        for earlier in bits:
            if earlier < bit:
                part_copy(mask | earlier, earlier).wait_recv()
                value = value + part_got[mask | earlier].astype(jnp.float32)
        part_send[mask] = value.astype(jnp.bfloat16)
        part_copy(mask, bit).start()
    value = project(0)
    for bit in bits:
        part_copy(bit, bit).wait_recv()
        value = value + part_got[bit].astype(jnp.float32)
    stream = (res[...].astype(jnp.float32) + value.astype(jnp.bfloat16).astype(jnp.float32)).astype(
        jnp.bfloat16
    )
    stream_ref[...] = stream
    wide = stream.astype(jnp.float32)
    scale = lax.rsqrt(jnp.mean(wide * wide, axis=-1, keepdims=True) + EPS)
    normed_ref[...] = (wide * scale * gain[...]).astype(jnp.bfloat16)
    for mask in order:
        part_copy(mask, low_bit(mask)).wait_send()


def mixer(n_sp, n_tp, args, residual, norm_gain):
    q1, k1, v1, g1, d1, norm1, out1, q2, k2, v2, g2, d2, norm2, out2 = args
    length = q1.shape[0]
    blocks = length // BLOCK
    count = (q1.shape[1] + q2.shape[1]) // 128
    heads = (v1.shape[1] + v2.shape[1]) // VALUE_W
    rows, width = residual.shape
    packed = count * (VALUE_W + 16)
    bf, f32 = jnp.bfloat16, jnp.float32
    vmem = pl.BlockSpec(memory_space=pltpu.VMEM)
    sem = pltpu.SemaphoreType.DMA
    return pl.pallas_call(
        functools.partial(mixer_kernel, n_sp, n_tp),
        out_shape=(jax.ShapeDtypeStruct((rows, width), bf),) * 2,
        in_specs=[vmem] * 16,
        out_specs=(vmem, vmem),
        scratch_shapes=[
            pltpu.VMEM((count, length, 128), f32),
            pltpu.VMEM((2, count, length, 128), bf),
            pltpu.VMEM((2, count, length, 128), bf),
            pltpu.VMEM((2, count, blocks, VALUE_W, 128), f32),
            pltpu.VMEM((2, count, -(-blocks // 8) * 8, 128), f32),
            pltpu.VMEM((2, packed, 128), bf),
            pltpu.VMEM((n_sp, packed, 128), bf),
            pltpu.VMEM((2, count, VALUE_W, 128), f32),
            pltpu.VMEM((heads, length, VALUE_W), f32),
            pltpu.VMEM((length, heads * VALUE_W), bf),
            pltpu.VMEM((n_tp, rows, width), bf),
            pltpu.VMEM((n_tp, rows, width), bf),
            sem((n_sp,)),
            sem((n_sp,)),
            sem((n_tp,)),
            sem((n_tp,)),
        ],
        compiler_params=pltpu.CompilerParams(
            collective_id=0, has_side_effects=True, vmem_limit_bytes=60 * 2**20
        ),
    )(
        q1, k1, v1, g1, d1, q2, k2, v2, g2, d2,
        norm1[None], norm2[None], out1, out2, residual, norm_gain[None],
    )


def expert_kernel(
    stride, span, stream, normed, weight, slot, w_gate, w_up, w_down, out_ref,
    v_gate, v_up, v_down, z_send, z_got, data, part, from_core, from_x, from_y, back_got,
    w_sem, s_sem, r_sem,
):
    sp, tp = lax.axis_index("sp"), lax.axis_index("tp")
    width = normed.shape[1]
    half = (data.shape[1] // 32 + 1) * 16 if (data.shape[1] // 16) % 2 else data.shape[1] // 2
    top, low = slice(0, half), slice(half, data.shape[1])
    place, side = sp // 2, lax.rem(sp, 2)
    core, across, along = (sp, flip_bit(tp, 1)), (sp, flip_bit(tp, 2)), (flip_bit(sp, 1), tp)
    far = [(lax.rem(place + off, GROUPS), off) for off in range(1, GROUPS)]
    loads = [
        pltpu.make_async_copy(source, target, w_sem.at[i])
        for i, (source, target) in enumerate(((w_gate, v_gate), (w_up, v_up), (w_down, v_down)))
    ]
    for load in loads:
        load.start()
    meet([(z * 2 + side, tp) for z, _ in far] + [core, across, along])

    def copy(number, source, target, device):
        return pltpu.make_async_remote_copy(
            src_ref=source,
            dst_ref=target,
            send_sem=s_sem.at[number],
            recv_sem=r_sem.at[number],
            device_id=device,
            device_id_type=MESH,
        )

    rows = slot.shape[1]
    spread = (
        lax.broadcasted_iota(jnp.int32, (GROUPS * span, rows), 0) == slot[...]
    ).astype(jnp.float32).astype(jnp.bfloat16)
    high = weight[...].astype(jnp.bfloat16)
    rest = (weight[...] - high.astype(jnp.float32)).astype(jnp.bfloat16)
    z_send[:, :width] = contract(spread, normed[...], NN).astype(jnp.bfloat16)
    z_send[:, width : width + 128] = contract(spread, high, NN).astype(jnp.bfloat16)
    z_send[:, width + 128 :] = contract(spread, rest, NN).astype(jnp.bfloat16)

    def block(index):
        return pl.ds(pl.multiple_of(index * span, 16), span)

    def turn(index):
        return pl.ds(pl.multiple_of(index * stride, 16), span)

    outs = [copy(off, z_send.at[block(z)], z_got.at[off], (z * 2 + side, tp)) for z, off in far]
    for one in outs:
        one.start()
    data[0] = jnp.zeros(data.shape[1:], jnp.bfloat16)
    data[0, turn(place), :] = z_send[block(place), :]
    for one, (_, off) in zip(outs, far):
        one.wait()
        source = lax.rem(place - off + GROUPS, GROUPS)
        data[0, turn(source), :] = data[0, turn(source), :] + z_got[off]

    base = GROUPS
    c_0 = copy(base, data.at[0], data.at[1], core)
    a_y = copy(base + 1, data.at[0, top], data.at[2, top], along)
    b_x = copy(base + 2, data.at[0, low], data.at[4, low], across)
    a_x = copy(base + 3, data.at[0, top], data.at[4, top], across)
    b_y = copy(base + 4, data.at[0, low], data.at[2, low], along)
    a_d = copy(base + 5, data.at[2, top], data.at[6, top], across)
    b_d = copy(base + 6, data.at[4, low], data.at[6, low], along)
    c_y = copy(base + 7, data.at[2], data.at[3], core)
    c_x = copy(base + 8, data.at[4], data.at[5], core)
    c_d = copy(base + 9, data.at[6], data.at[7], core)
    base += 10
    p_c = [copy(base + i, part.at[2 * i + 1], from_core.at[i], core) for i in range(4)]
    base += 4
    r_ax = copy(base, part.at[4, top], from_x.at[0, top], across)
    r_by = copy(base + 1, part.at[2, low], from_y.at[0, low], along)
    r_ad = copy(base + 2, part.at[6, top], from_x.at[1, top], across)
    r_bd = copy(base + 3, part.at[6, low], from_y.at[1, low], along)
    r_ay = copy(base + 4, part.at[2, top], from_y.at[0, top], along)
    r_bx = copy(base + 5, part.at[4, low], from_x.at[0, low], across)
    base += 6
    for one in (a_y, b_x, a_x, b_y, c_0):
        one.start()

    for load in loads:
        load.wait()

    def compute(first, count):
        @pl.loop(first, first + count)
        def _(m):
            x = data[m, :, :width]
            w = data[m, :, width : width + 128].astype(jnp.float32) + data[
                m, :, width + 128 :
            ].astype(jnp.float32)
            lane = lax.broadcasted_iota(jnp.int32, w.shape, 1)
            w = jnp.sum(jnp.where(lane == side, w, 0.0), axis=1, keepdims=True)
            gate = contract(x, v_gate[...], NN)
            up = contract(x, v_up[...], NN)
            hidden = (gate / (1.0 + jnp.exp(-gate)) * up * w).astype(jnp.bfloat16)
            part[m] = contract(hidden, v_down[...], NN).astype(jnp.bfloat16)

    def add(m, where, term):
        part[m, where, :] = (
            part[m, where, :].astype(jnp.float32) + term.astype(jnp.float32)
        ).astype(jnp.bfloat16)

    everything = slice(0, data.shape[1])
    c_0.wait_recv()
    compute(0, 2)
    p_c[0].start()
    a_y.wait_recv()
    a_d.start()
    b_x.wait_recv()
    b_d.start()
    b_y.wait_recv()
    c_y.start()
    a_x.wait_recv()
    c_x.start()
    c_y.wait_recv()
    c_x.wait_recv()
    compute(2, 4)
    p_c[1].start()
    p_c[2].start()
    p_c[1].wait_recv()
    add(2, everything, from_core[1])
    r_by.start()
    p_c[2].wait_recv()
    add(4, everything, from_core[2])
    r_ax.start()
    a_d.wait_recv()
    b_d.wait_recv()
    c_d.start()
    c_d.wait_recv()
    compute(6, 2)
    p_c[3].start()
    p_c[3].wait_recv()
    add(6, everything, from_core[3])
    r_ad.start()
    r_bd.start()
    p_c[0].wait_recv()
    r_ad.wait_recv()
    add(2, top, from_x[1, top])
    r_ay.start()
    r_bd.wait_recv()
    add(4, low, from_y[1, low])
    r_bx.start()
    r_ax.wait_recv()
    r_by.wait_recv()
    r_ay.wait_recv()
    r_bx.wait_recv()
    f32 = jnp.float32
    summed = part[0].astype(f32) + from_core[0].astype(f32)
    part[0] = (summed + from_x[0].astype(f32) + from_y[0].astype(f32)).astype(jnp.bfloat16)

    outs = []
    for z, off in far:
        outs.append(copy(base + off, part.at[0, turn(z)], back_got.at[block(place)], (z * 2 + side, tp)))
        outs[-1].start()
    back_got[block(place), :] = part[0, turn(place), :]
    for one in outs:
        one.wait_recv()
    picked = contract(spread, back_got[...], TN)
    out_ref[...] = (stream[...].astype(f32) + picked).astype(jnp.bfloat16)
    for one in [c_0, a_y, b_x, a_x, b_y, a_d, b_d, c_y, c_x, c_d] + p_c + outs:
        one.wait_send()
    for one in (r_ax, r_by, r_ad, r_bd, r_ay, r_bx):
        one.wait_send()


def grouped_experts(stream, normed, routes, weights, capacity, w_gate, w_up, w_down):
    rows, width = stream.shape
    stride = (capacity - 1) // 16 * 16
    if stride + 1 < capacity:
        stride += 16
    span = -(-(capacity + (GROUPS - 1) * max(0, capacity - stride)) // 16) * 16
    length = stride * (GROUPS - 1) + span
    group = routes[:, 0] // 2
    position = jnp.arange(rows, dtype=jnp.int32)
    ahead = (group[:, None] == group[None, :]) & (position[None, :] < position[:, None])
    nth = jnp.sum(ahead.astype(jnp.int32), axis=1)
    shift = lax.axis_index("sp") // 2 * max(0, capacity - stride)
    slot = (group * span + shift + nth)[None, :]
    side = routes[:, :, None] % 2 == jnp.arange(128, dtype=jnp.int32)[None, None, :]
    weight = jnp.sum(jnp.where(side, weights[:, :, None], 0.0), axis=1)
    bf = jnp.bfloat16
    vmem = pl.BlockSpec(memory_space=pltpu.VMEM)
    hbm = pl.BlockSpec(memory_space=pl.ANY)
    sem = pltpu.SemaphoreType.DMA
    wide = width + 256
    copies = 2 * GROUPS + 20
    return pl.pallas_call(
        functools.partial(expert_kernel, stride, span),
        out_shape=jax.ShapeDtypeStruct((rows, width), bf),
        in_specs=[vmem] * 4 + [hbm] * 3,
        out_specs=vmem,
        scratch_shapes=[
            pltpu.VMEM(w_gate.shape, bf),
            pltpu.VMEM(w_up.shape, bf),
            pltpu.VMEM(w_down.shape, bf),
            pltpu.VMEM((GROUPS * span, wide), bf),
            pltpu.VMEM((GROUPS, span, wide), bf),
            pltpu.VMEM((8, length, wide), bf),
            pltpu.VMEM((8, length, width), bf),
            pltpu.VMEM((4, length, width), bf),
            pltpu.VMEM((2, length, width), bf),
            pltpu.VMEM((2, length, width), bf),
            pltpu.VMEM((GROUPS * span, width), bf),
            sem((3,)),
            sem((copies,)),
            sem((copies,)),
        ],
        compiler_params=pltpu.CompilerParams(
            collective_id=1, has_side_effects=True, vmem_limit_bytes=60 * 2**20
        ),
    )(stream, normed, weight, slot, w_gate, w_up, w_down)


def slot_table(routes, capacity, experts):
    flat = routes.reshape(-1)
    count = flat.shape[0]
    onehot = (flat[:, None] == jnp.arange(experts, dtype=jnp.int32)[None, :]).astype(jnp.int32)
    place = jnp.sum((jnp.cumsum(onehot, axis=0) - onehot) * onehot, axis=1)
    table = (
        jnp.full((experts, capacity), count, jnp.int32)
        .at[flat, place]
        .set(jnp.arange(count, dtype=jnp.int32))
    )
    return (table, place)


def body(
    residual,
    query_one,
    key_one,
    value_one,
    gate_one,
    decay_one,
    norm_one,
    output_one,
    query_two,
    key_two,
    value_two,
    gate_two,
    decay_two,
    norm_two,
    output_two,
    norm_gain,
    expert_ids,
    group_weight,
    pair_weight,
    expert_gate,
    expert_up,
    expert_down,
):
    stream, normed_rows = mixer(
        lax.axis_size("sp"),
        lax.axis_size("tp"),
        (
            query_one, key_one, value_one, gate_one, decay_one, norm_one, output_one,
            query_two, key_two, value_two, gate_two, decay_two, norm_two, output_two,
        ),
        residual,
        norm_gain,
    )
    rows_dev = residual.shape[0]
    rank = lax.axis_index("tp")
    experts = lax.axis_size("sp")
    capacity = max(2, 2 * rows_dev // (experts - GROUPS) + 1)
    own_routes = lax.dynamic_slice_in_dim(expert_ids, rank * rows_dev, rows_dev, 0)
    own_group = lax.dynamic_slice_in_dim(group_weight, rank * rows_dev, rows_dev, 0)
    own_pair = lax.dynamic_slice_in_dim(pair_weight, rank * rows_dev, rows_dev, 0)
    weights = own_group[:, None] * own_pair / jnp.sum(own_pair, axis=1, keepdims=True)
    if experts == 2 * GROUPS and lax.axis_size("tp") == 4:
        return grouped_experts(
            stream,
            normed_rows,
            own_routes,
            weights,
            capacity,
            expert_gate[0],
            expert_up[0],
            expert_down[0],
        )
    blank = jnp.zeros((1, D), jnp.bfloat16)
    table, own_place = slot_table(own_routes, capacity, experts)
    index = jnp.where(table == 2 * rows_dev, rows_dev, table // 2)
    send = jnp.concatenate([normed_rows, blank], axis=0)[index][None]
    received = lax.all_to_all(send, "sp", split_axis=1, concat_axis=1, tiled=True)
    received = lax.all_gather(received, "tp", axis=0, tiled=True)
    flat = received.reshape(-1, received.shape[-1])
    gate_part = jnp.dot(flat, expert_gate[0], preferred_element_type=jnp.float32)
    up_part = jnp.dot(flat, expert_up[0], preferred_element_type=jnp.float32)
    hidden = (jax.nn.silu(gate_part) * up_part).astype(jnp.bfloat16)
    share_sum = lax.psum_scatter(
        jnp.dot(hidden, expert_down[0], preferred_element_type=jnp.float32)
        .reshape(received.shape)
        .astype(jnp.bfloat16),
        "tp",
        scatter_dimension=0,
        tiled=True,
    )
    returned = lax.all_to_all(share_sum, "sp", split_axis=1, concat_axis=1, tiled=True)
    slot_index = own_routes.reshape(-1) * capacity + own_place
    picked = returned.reshape(-1, D)[slot_index].astype(jnp.float32).reshape(rows_dev, 2, D)
    layer = stream.astype(jnp.float32) + jnp.sum(weights[:, :, None] * picked, axis=1)
    return layer.astype(jnp.bfloat16)


def solution(mesh):
    placed = (
        P(("sp", "tp"), None),
        P("sp", "tp"),
        P("sp", "tp"),
        P("sp", "tp"),
        P("sp", "tp"),
        P(None, "sp", "tp"),
        P(),
        P("tp", None),
        P("sp", "tp"),
        P("sp", "tp"),
        P("sp", "tp"),
        P("sp", "tp"),
        P(None, "sp", "tp"),
        P(),
        P("tp", None),
        P(),
        P("sp", None),
        P("sp"),
        P("sp", None),
        P("sp", None, "tp"),
        P("sp", None, "tp"),
        P("sp", "tp", None),
    )
    return jax.shard_map(
        body, mesh=mesh, in_specs=placed, out_specs=P(("sp", "tp"), None), check_vma=False
    )
```

```python
import functools

import jax
import jax.numpy as jnp
from jax import lax
from jax.experimental import pallas as pl
from jax.experimental.pallas import tpu as pltpu
from jax.sharding import PartitionSpec as P

D = 2048
KEY_ONE = 64
KEY_TWO = 128
VALUE_W = 128
BLOCK = 64
GROUPS = 4


MESH = pl.DeviceIdType.MESH
TAU = 16.0
EPS = 1e-06


def log_sigmoid(x):
    return jnp.minimum(x, 0.0) - jnp.log1p(jnp.exp(-jnp.abs(x)))


def contract(a, b, dims):
    return lax.dot_general(a, b, (dims, ((), ())), preferred_element_type=jnp.float32)


NN, NT, TN = ((1,), (0,)), ((1,), (1,)), ((0,), (0,))


def flip_bit(index, bit):
    return index + bit - 2 * bit * lax.rem(index // bit, 2)


def meet(peers):
    barrier = pltpu.get_barrier_semaphore()
    for peer in peers:
        pl.semaphore_signal(barrier, inc=1, device_id=peer, device_id_type=MESH)
    pl.semaphore_wait(barrier, len(peers))


def mixer_kernel(
    n_sp,
    n_tp,
    q1,
    k1,
    v1,
    g1,
    d1,
    q2,
    k2,
    v2,
    g2,
    d2,
    norm1,
    norm2,
    out1,
    out2,
    res,
    gain,
    stream_ref,
    normed_ref,
    cum,
    qd,
    kd,
    added,
    ends,
    sent,
    got,
    carried,
    total,
    mixed,
    part_send,
    part_got,
    st_send,
    st_recv,
    pt_send,
    pt_recv,
):
    sp, tp = lax.axis_index("sp"), lax.axis_index("tp")
    length = q1.shape[0]
    blocks = length // BLOCK
    lanes = 128
    units = []
    for q, k, v, g, d, norm, key in (
        (q1, k1, v1, g1, d1, norm1, KEY_ONE),
        (q2, k2, v2, g2, d2, norm2, KEY_TWO),
    ):
        per = lanes // key
        for at in range(q.shape[1] // lanes):
            units.append((q, k, v, g, d, norm, key, per, at))
    count = len(units)
    bits = [1 << r for r in range(n_tp.bit_length() - 1)]

    meet(
        [(lax.rem(sp + off, n_sp), tp) for off in range(1, n_sp)]
        + [(sp, flip_bit(tp, bit)) for bit in bits]
    )

    t_at = lax.broadcasted_iota(jnp.int32, (length, length), 0)
    s_at = lax.broadcasted_iota(jnp.int32, (length, length), 1)
    same = (t_at // BLOCK) == (s_at // BLOCK)
    for way in range(2):
        tri = jnp.where(same & ((s_at <= t_at) if way == 0 else (s_at >= t_at)), 1.0, 0.0).astype(
            jnp.bfloat16
        )
        for u, (q, k, v, g, d, norm, key, per, at) in enumerate(units):
            cols = slice(at * lanes, (at + 1) * lanes)
            rate = log_sigmoid(d[way, :, cols].astype(jnp.float32)) / TAU
            high = rate.astype(jnp.bfloat16)
            rest = rate - high.astype(jnp.float32)
            mid = rest.astype(jnp.bfloat16)
            low = (rest - mid.astype(jnp.float32)).astype(jnp.bfloat16)
            cum[u] = contract(tri, high, NN) + contract(tri, mid, NN) + contract(tri, low, NN)
            state = jnp.zeros((VALUE_W, lanes), jnp.float32)
            reach = jnp.zeros((1, lanes), jnp.float32)
            lane = lax.broadcasted_iota(jnp.int32, (VALUE_W, lanes), 1) // key
            for n in range(blocks) if way == 0 else range(blocks - 1, -1, -1):
                rows = slice(n * BLOCK, (n + 1) * BLOCK)
                c = cum[u, rows, :]
                e = c[BLOCK - 1 : BLOCK] if way == 0 else c[0:1]
                queries = q[rows, cols].astype(jnp.float32) * key ** (-0.5)
                keys = k[rows, cols].astype(jnp.float32)
                qd[way, u, rows, :] = (queries * jnp.exp(c)).astype(jnp.bfloat16)
                kd[way, u, rows, :] = (keys * jnp.exp(-c)).astype(jnp.bfloat16)
                end = (keys * jnp.exp(e - c)).astype(jnp.bfloat16)
                term = None
                for h in range(per):
                    head = at * per + h
                    value = v[rows, head * VALUE_W : (head + 1) * VALUE_W]
                    new = contract(value, end, TN)
                    term = new if term is None else jnp.where(lane == h, new, term)
                added[way, u, n] = term
                fade = jnp.exp(e)
                ends[way, u, n : n + 1, :] = fade
                state = state * fade + term
                reach = reach + e
            sent[way, u * VALUE_W : (u + 1) * VALUE_W, :] = state.astype(jnp.bfloat16)
            sent[way, count * VALUE_W + 16 * u : count * VALUE_W + 16 * (u + 1), :] = (
                jnp.broadcast_to(jnp.exp(reach), (16, lanes)).astype(jnp.bfloat16)
            )

    def state_copy(off):
        to = lax.rem(sp + off, n_sp)
        way = jnp.where(to > sp, 0, 1)
        return pltpu.make_async_remote_copy(
            src_ref=sent.at[way],
            dst_ref=got.at[off],
            send_sem=st_send.at[off],
            recv_sem=st_recv.at[off],
            device_id=(to, tp),
            device_id_type=MESH,
        )

    @pl.loop(1, n_sp)
    def _(off):
        state_copy(off).start()

    t_blk = lax.broadcasted_iota(jnp.int32, (BLOCK, BLOCK), 0)
    s_blk = lax.broadcasted_iota(jnp.int32, (BLOCK, BLOCK), 1)
    first = 0
    for u, (q, k, v, g, d, norm, key, per, at) in enumerate(units):
        lane = lax.broadcasted_iota(jnp.int32, (BLOCK, lanes), 1) // key
        for h in range(per):
            head = at * per + h
            for n in range(blocks):
                rows = slice(n * BLOCK, (n + 1) * BLOCK)
                scores = None
                for way in range(2):
                    queries = qd[way, u, rows, :]
                    if per > 1:
                        queries = jnp.where(lane == h, queries, jnp.zeros_like(queries))
                    one = contract(queries, kd[way, u, rows, :], NT)
                    one = jnp.where((s_blk <= t_blk) if way == 0 else (s_blk >= t_blk), one, 0.0)
                    scores = one if scores is None else scores + one
                value = v[rows, head * VALUE_W : (head + 1) * VALUE_W]
                total[first + h, rows, :] = contract(scores.astype(jnp.bfloat16), value, NN)
        first += per

    @pl.loop(1, n_sp)
    def _(off):
        state_copy(off).wait()

    carried[...] = jnp.zeros_like(carried)

    def fold(way, who):
        off = lax.rem(sp - who + n_sp, n_sp)
        for u in range(count):
            fade = got[off, count * VALUE_W + 16 * u : count * VALUE_W + 16 * (u + 1), :][0:1]
            state = got[off, u * VALUE_W : (u + 1) * VALUE_W, :]
            carried[way, u] = carried[way, u] * fade.astype(jnp.float32) + state.astype(jnp.float32)

    @pl.loop(0, sp)
    def _(who):
        fold(0, who)

    @pl.loop(0, n_sp - 1 - sp)
    def _(back):
        fold(1, n_sp - 1 - back)

    first = 0
    for u, (q, k, v, g, d, norm, key, per, at) in enumerate(units):
        lane = lax.broadcasted_iota(jnp.int32, (BLOCK, lanes), 1) // key
        for way in range(2):
            state = carried[way, u]
            for n in range(blocks) if way == 0 else range(blocks - 1, -1, -1):
                rows = slice(n * BLOCK, (n + 1) * BLOCK)
                low = state.astype(jnp.bfloat16)
                for h in range(per):
                    queries = qd[way, u, rows, :]
                    if per > 1:
                        queries = jnp.where(lane == h, queries, jnp.zeros_like(queries))
                    total[first + h, rows, :] += contract(queries, low, NT)
                state = state * ends[way, u, n : n + 1, :] + added[way, u, n]
        for h in range(per):
            head = at * per + h
            cols = slice(head * VALUE_W, (head + 1) * VALUE_W)
            x = total[first + h]
            y = x * lax.rsqrt(jnp.mean(x * x, axis=-1, keepdims=True) + EPS) * norm[...]
            gate = g[:, cols].astype(jnp.float32)
            y = y * (gate / (1.0 + jnp.exp(-gate)))
            mixed[:, (first + h) * VALUE_W : (first + h + 1) * VALUE_W] = y.astype(jnp.bfloat16)
        first += per

    rows_dev = res.shape[0]
    split = out1.shape[0]

    def project(mask):
        block = tp
        for bit in bits:
            if mask & bit:
                block = flip_bit(block, bit)
        rows = pl.ds(pl.multiple_of(block * rows_dev, 16), rows_dev)
        return contract(mixed[rows, :split], out1[...], NN) + contract(
            mixed[rows, split:], out2[...], NN
        )

    def part_copy(mask, bit):
        return pltpu.make_async_remote_copy(
            src_ref=part_send.at[mask],
            dst_ref=part_got.at[mask],
            send_sem=pt_send.at[mask],
            recv_sem=pt_recv.at[mask],
            device_id=(sp, flip_bit(tp, bit)),
            device_id_type=MESH,
        )

    low_bit = lambda m: m & -m
    order = sorted(range(1, n_tp), key=lambda m: (low_bit(m), -m))
    for mask in order:
        bit = low_bit(mask)
        value = project(mask)
        for earlier in bits:
            if earlier < bit:
                part_copy(mask | earlier, earlier).wait_recv()
                value = value + part_got[mask | earlier].astype(jnp.float32)
        part_send[mask] = value.astype(jnp.bfloat16)
        part_copy(mask, bit).start()
    value = project(0)
    for bit in bits:
        part_copy(bit, bit).wait_recv()
        value = value + part_got[bit].astype(jnp.float32)
    stream = (res[...].astype(jnp.float32) + value.astype(jnp.bfloat16).astype(jnp.float32)).astype(
        jnp.bfloat16
    )
    stream_ref[...] = stream
    wide = stream.astype(jnp.float32)
    scale = lax.rsqrt(jnp.mean(wide * wide, axis=-1, keepdims=True) + EPS)
    normed_ref[...] = (wide * scale * gain[...]).astype(jnp.bfloat16)
    for mask in order:
        part_copy(mask, low_bit(mask)).wait_send()


def mixer(n_sp, n_tp, args, residual, norm_gain):
    q1, k1, v1, g1, d1, norm1, out1, q2, k2, v2, g2, d2, norm2, out2 = args
    length = q1.shape[0]
    blocks = length // BLOCK
    count = (q1.shape[1] + q2.shape[1]) // 128
    heads = (v1.shape[1] + v2.shape[1]) // VALUE_W
    rows, width = residual.shape
    packed = count * (VALUE_W + 16)
    bf, f32 = jnp.bfloat16, jnp.float32
    vmem = pl.BlockSpec(memory_space=pltpu.VMEM)
    sem = pltpu.SemaphoreType.DMA
    return pl.pallas_call(
        functools.partial(mixer_kernel, n_sp, n_tp),
        out_shape=(jax.ShapeDtypeStruct((rows, width), bf),) * 2,
        in_specs=[vmem] * 16,
        out_specs=(vmem, vmem),
        scratch_shapes=[
            pltpu.VMEM((count, length, 128), f32),
            pltpu.VMEM((2, count, length, 128), bf),
            pltpu.VMEM((2, count, length, 128), bf),
            pltpu.VMEM((2, count, blocks, VALUE_W, 128), f32),
            pltpu.VMEM((2, count, -(-blocks // 8) * 8, 128), f32),
            pltpu.VMEM((2, packed, 128), bf),
            pltpu.VMEM((n_sp, packed, 128), bf),
            pltpu.VMEM((2, count, VALUE_W, 128), f32),
            pltpu.VMEM((heads, length, VALUE_W), f32),
            pltpu.VMEM((length, heads * VALUE_W), bf),
            pltpu.VMEM((n_tp, rows, width), bf),
            pltpu.VMEM((n_tp, rows, width), bf),
            sem((n_sp,)),
            sem((n_sp,)),
            sem((n_tp,)),
            sem((n_tp,)),
        ],
        compiler_params=pltpu.CompilerParams(
            collective_id=0, has_side_effects=True, vmem_limit_bytes=60 * 2**20
        ),
    )(
        q1, k1, v1, g1, d1, q2, k2, v2, g2, d2,
        norm1[None], norm2[None], out1, out2, residual, norm_gain[None],
    )


def expert_kernel(
    stride, span, stream, normed, weight, slot, w_gate, w_up, w_down, out_ref,
    v_gate, v_up, v_down, z_send, z_got, data, part, from_core, from_x, from_y, back_got,
    w_sem, s_sem, r_sem,
):
    sp, tp = lax.axis_index("sp"), lax.axis_index("tp")
    width = normed.shape[1]
    half = (data.shape[1] // 32 + 1) * 16 if (data.shape[1] // 16) % 2 else data.shape[1] // 2
    top, low = slice(0, half), slice(half, data.shape[1])
    place, side = sp // 2, lax.rem(sp, 2)
    core, across, along = (sp, flip_bit(tp, 1)), (sp, flip_bit(tp, 2)), (flip_bit(sp, 1), tp)
    far = [(lax.rem(place + off, GROUPS), off) for off in range(1, GROUPS)]
    loads = [
        pltpu.make_async_copy(source, target, w_sem.at[i])
        for i, (source, target) in enumerate(((w_gate, v_gate), (w_up, v_up), (w_down, v_down)))
    ]
    for load in loads:
        load.start()
    meet([(z * 2 + side, tp) for z, _ in far] + [core, across, along])

    def copy(number, source, target, device):
        return pltpu.make_async_remote_copy(
            src_ref=source,
            dst_ref=target,
            send_sem=s_sem.at[number],
            recv_sem=r_sem.at[number],
            device_id=device,
            device_id_type=MESH,
        )

    rows = slot.shape[1]
    spread = (
        lax.broadcasted_iota(jnp.int32, (GROUPS * span, rows), 0) == slot[...]
    ).astype(jnp.float32).astype(jnp.bfloat16)
    high = weight[...].astype(jnp.bfloat16)
    rest = (weight[...] - high.astype(jnp.float32)).astype(jnp.bfloat16)
    z_send[:, :width] = contract(spread, normed[...], NN).astype(jnp.bfloat16)
    second = lax.broadcasted_iota(jnp.int32, high.shape, 1) >= 64
    both = jnp.where(second, rest.astype(jnp.float32), high.astype(jnp.float32))
    z_send[:, width:] = contract(spread, both.astype(jnp.bfloat16), NN).astype(jnp.bfloat16)

    def block(index):
        return pl.ds(pl.multiple_of(index * span, 16), span)

    def turn(index):
        return pl.ds(pl.multiple_of(index * stride, 16), span)

    outs = [copy(off, z_send.at[block(z)], z_got.at[off], (z * 2 + side, tp)) for z, off in far]
    for one in outs:
        one.start()
    data[0] = jnp.zeros(data.shape[1:], jnp.bfloat16)
    data[0, turn(place), :] = z_send[block(place), :]
    for one, (_, off) in zip(outs, far):
        one.wait()
        source = lax.rem(place - off + GROUPS, GROUPS)
        data[0, turn(source), :] = data[0, turn(source), :] + z_got[off]

    base = GROUPS
    c_0 = copy(base, data.at[0], data.at[1], core)
    a_y = copy(base + 1, data.at[0, top], data.at[2, top], along)
    b_x = copy(base + 2, data.at[0, low], data.at[4, low], across)
    a_x = copy(base + 3, data.at[0, top], data.at[4, top], across)
    b_y = copy(base + 4, data.at[0, low], data.at[2, low], along)
    a_d = copy(base + 5, data.at[2, top], data.at[6, top], across)
    b_d = copy(base + 6, data.at[4, low], data.at[6, low], along)
    c_y = copy(base + 7, data.at[2], data.at[3], core)
    c_x = copy(base + 8, data.at[4], data.at[5], core)
    c_d = copy(base + 9, data.at[6], data.at[7], core)
    base += 10
    p_c = [copy(base + i, part.at[2 * i + 1], from_core.at[i], core) for i in range(4)]
    base += 4
    r_ax = copy(base, part.at[4, top], from_x.at[0, top], across)
    r_by = copy(base + 1, part.at[2, low], from_y.at[0, low], along)
    r_ad = copy(base + 2, part.at[6, top], from_x.at[1, top], across)
    r_bd = copy(base + 3, part.at[6, low], from_y.at[1, low], along)
    r_ay = copy(base + 4, part.at[2, top], from_y.at[0, top], along)
    r_bx = copy(base + 5, part.at[4, low], from_x.at[0, low], across)
    base += 6
    for one in (a_y, b_x, a_x, b_y, c_0):
        one.start()

    for load in loads:
        load.wait()

    def compute(first, count):
        @pl.loop(first, first + count)
        def _(m):
            x = data[m, :, :width]
            w = data[m, :, width:].astype(jnp.float32)
            lane = lax.broadcasted_iota(jnp.int32, w.shape, 1)
            w = jnp.sum(jnp.where((lane == side) | (lane == side + 64), w, 0.0), axis=1, keepdims=True)
            gate = contract(x, v_gate[...], NN)
            up = contract(x, v_up[...], NN)
            hidden = (gate / (1.0 + jnp.exp(-gate)) * up * w).astype(jnp.bfloat16)
            part[m] = contract(hidden, v_down[...], NN).astype(jnp.bfloat16)

    def add(m, where, term):
        part[m, where, :] = (
            part[m, where, :].astype(jnp.float32) + term.astype(jnp.float32)
        ).astype(jnp.bfloat16)

    everything = slice(0, data.shape[1])
    c_0.wait_recv()
    compute(0, 2)
    p_c[0].start()
    a_y.wait_recv()
    a_d.start()
    b_x.wait_recv()
    b_d.start()
    b_y.wait_recv()
    c_y.start()
    a_x.wait_recv()
    c_x.start()
    c_y.wait_recv()
    c_x.wait_recv()
    compute(2, 4)
    p_c[1].start()
    p_c[2].start()
    p_c[1].wait_recv()
    add(2, everything, from_core[1])
    r_by.start()
    p_c[2].wait_recv()
    add(4, everything, from_core[2])
    r_ax.start()
    a_d.wait_recv()
    b_d.wait_recv()
    c_d.start()
    compute(6, 1)
    c_d.wait_recv()
    compute(7, 1)
    p_c[3].start()
    p_c[3].wait_recv()
    add(6, everything, from_core[3])
    r_ad.start()
    r_bd.start()
    p_c[0].wait_recv()
    r_ad.wait_recv()
    add(2, top, from_x[1, top])
    r_ay.start()
    r_bd.wait_recv()
    add(4, low, from_y[1, low])
    r_bx.start()
    r_ax.wait_recv()
    r_by.wait_recv()
    r_ay.wait_recv()
    r_bx.wait_recv()
    f32 = jnp.float32
    summed = part[0].astype(f32) + from_core[0].astype(f32)
    part[0] = (summed + from_x[0].astype(f32) + from_y[0].astype(f32)).astype(jnp.bfloat16)

    outs = []
    for z, off in far:
        outs.append(copy(base + off, part.at[0, turn(z)], back_got.at[block(place)], (z * 2 + side, tp)))
        outs[-1].start()
    back_got[block(place), :] = part[0, turn(place), :]
    for one in outs:
        one.wait_recv()
    picked = contract(spread, back_got[...], TN)
    out_ref[...] = (stream[...].astype(f32) + picked).astype(jnp.bfloat16)
    for one in [c_0, a_y, b_x, a_x, b_y, a_d, b_d, c_y, c_x, c_d] + p_c + outs:
        one.wait_send()
    for one in (r_ax, r_by, r_ad, r_bd, r_ay, r_bx):
        one.wait_send()


def grouped_experts(stream, normed, routes, weights, capacity, w_gate, w_up, w_down):
    rows, width = stream.shape
    stride = (capacity - 1) // 16 * 16
    if stride + 1 < capacity:
        stride += 16
    span = -(-(capacity + (GROUPS - 1) * max(0, capacity - stride)) // 16) * 16
    length = stride * (GROUPS - 1) + span
    group = routes[:, 0] // 2
    position = jnp.arange(rows, dtype=jnp.int32)
    ahead = (group[:, None] == group[None, :]) & (position[None, :] < position[:, None])
    nth = jnp.sum(ahead.astype(jnp.int32), axis=1)
    shift = lax.axis_index("sp") // 2 * max(0, capacity - stride)
    slot = (group * span + shift + nth)[None, :]
    side = routes[:, :, None] % 2 == (jnp.arange(128, dtype=jnp.int32) % 64)[None, None, :]
    weight = jnp.sum(jnp.where(side, weights[:, :, None], 0.0), axis=1)
    bf = jnp.bfloat16
    vmem = pl.BlockSpec(memory_space=pltpu.VMEM)
    hbm = pl.BlockSpec(memory_space=pl.ANY)
    sem = pltpu.SemaphoreType.DMA
    wide = width + 128
    copies = 2 * GROUPS + 20
    return pl.pallas_call(
        functools.partial(expert_kernel, stride, span),
        out_shape=jax.ShapeDtypeStruct((rows, width), bf),
        in_specs=[vmem] * 4 + [hbm] * 3,
        out_specs=vmem,
        scratch_shapes=[
            pltpu.VMEM(w_gate.shape, bf),
            pltpu.VMEM(w_up.shape, bf),
            pltpu.VMEM(w_down.shape, bf),
            pltpu.VMEM((GROUPS * span, wide), bf),
            pltpu.VMEM((GROUPS, span, wide), bf),
            pltpu.VMEM((8, length, wide), bf),
            pltpu.VMEM((8, length, width), bf),
            pltpu.VMEM((4, length, width), bf),
            pltpu.VMEM((2, length, width), bf),
            pltpu.VMEM((2, length, width), bf),
            pltpu.VMEM((GROUPS * span, width), bf),
            sem((3,)),
            sem((copies,)),
            sem((copies,)),
        ],
        compiler_params=pltpu.CompilerParams(
            collective_id=1, has_side_effects=True, vmem_limit_bytes=60 * 2**20
        ),
    )(stream, normed, weight, slot, w_gate, w_up, w_down)


def slot_table(routes, capacity, experts):
    flat = routes.reshape(-1)
    count = flat.shape[0]
    onehot = (flat[:, None] == jnp.arange(experts, dtype=jnp.int32)[None, :]).astype(jnp.int32)
    place = jnp.sum((jnp.cumsum(onehot, axis=0) - onehot) * onehot, axis=1)
    table = (
        jnp.full((experts, capacity), count, jnp.int32)
        .at[flat, place]
        .set(jnp.arange(count, dtype=jnp.int32))
    )
    return (table, place)


def body(
    residual,
    query_one,
    key_one,
    value_one,
    gate_one,
    decay_one,
    norm_one,
    output_one,
    query_two,
    key_two,
    value_two,
    gate_two,
    decay_two,
    norm_two,
    output_two,
    norm_gain,
    expert_ids,
    group_weight,
    pair_weight,
    expert_gate,
    expert_up,
    expert_down,
):
    stream, normed_rows = mixer(
        lax.axis_size("sp"),
        lax.axis_size("tp"),
        (
            query_one, key_one, value_one, gate_one, decay_one, norm_one, output_one,
            query_two, key_two, value_two, gate_two, decay_two, norm_two, output_two,
        ),
        residual,
        norm_gain,
    )
    rows_dev = residual.shape[0]
    rank = lax.axis_index("tp")
    experts = lax.axis_size("sp")
    capacity = max(2, 2 * rows_dev // (experts - GROUPS) + 1)
    own_routes = lax.dynamic_slice_in_dim(expert_ids, rank * rows_dev, rows_dev, 0)
    own_group = lax.dynamic_slice_in_dim(group_weight, rank * rows_dev, rows_dev, 0)
    own_pair = lax.dynamic_slice_in_dim(pair_weight, rank * rows_dev, rows_dev, 0)
    weights = own_group[:, None] * own_pair / jnp.sum(own_pair, axis=1, keepdims=True)
    if experts == 2 * GROUPS and lax.axis_size("tp") == 4:
        return grouped_experts(
            stream,
            normed_rows,
            own_routes,
            weights,
            capacity,
            expert_gate[0],
            expert_up[0],
            expert_down[0],
        )
    blank = jnp.zeros((1, D), jnp.bfloat16)
    table, own_place = slot_table(own_routes, capacity, experts)
    index = jnp.where(table == 2 * rows_dev, rows_dev, table // 2)
    send = jnp.concatenate([normed_rows, blank], axis=0)[index][None]
    received = lax.all_to_all(send, "sp", split_axis=1, concat_axis=1, tiled=True)
    received = lax.all_gather(received, "tp", axis=0, tiled=True)
    flat = received.reshape(-1, received.shape[-1])
    gate_part = jnp.dot(flat, expert_gate[0], preferred_element_type=jnp.float32)
    up_part = jnp.dot(flat, expert_up[0], preferred_element_type=jnp.float32)
    hidden = (jax.nn.silu(gate_part) * up_part).astype(jnp.bfloat16)
    share_sum = lax.psum_scatter(
        jnp.dot(hidden, expert_down[0], preferred_element_type=jnp.float32)
        .reshape(received.shape)
        .astype(jnp.bfloat16),
        "tp",
        scatter_dimension=0,
        tiled=True,
    )
    returned = lax.all_to_all(share_sum, "sp", split_axis=1, concat_axis=1, tiled=True)
    slot_index = own_routes.reshape(-1) * capacity + own_place
    picked = returned.reshape(-1, D)[slot_index].astype(jnp.float32).reshape(rows_dev, 2, D)
    layer = stream.astype(jnp.float32) + jnp.sum(weights[:, :, None] * picked, axis=1)
    return layer.astype(jnp.bfloat16)


def solution(mesh):
    placed = (
        P(("sp", "tp"), None),
        P("sp", "tp"),
        P("sp", "tp"),
        P("sp", "tp"),
        P("sp", "tp"),
        P(None, "sp", "tp"),
        P(),
        P("tp", None),
        P("sp", "tp"),
        P("sp", "tp"),
        P("sp", "tp"),
        P("sp", "tp"),
        P(None, "sp", "tp"),
        P(),
        P("tp", None),
        P(),
        P("sp", None),
        P("sp"),
        P("sp", None),
        P("sp", None, "tp"),
        P("sp", None, "tp"),
        P("sp", "tp", None),
    )
    return jax.shard_map(
        body, mesh=mesh, in_specs=placed, out_specs=P(("sp", "tp"), None), check_vma=False
    )
```
